256 devices in a mesh: grp: 2 (over y), ep: 32 (over z, core), tp: 4 (over x).
Axes of the slice: x: 4, y: 2, z: 16, core: 2. Of those that a mesh axis runs over, the one named last changes fastest.
The devices are a block of a 4x16x16 slice.
Arguments:
- tokens: bfloat16 [32768, 2048], P(('grp', 'ep', 'tp')), parts along dimension 0, may hold values from -6 to 6
- norm_gain: float32 [2048], replicated, may hold values from 0.1 to 1.9
- route_ids: int32 [32768, 2], P(('grp', 'ep', 'tp')), parts along dimension 0, may hold values from 0 to 127, all different within a row; in each aligned block of 128 rows (0 to 127, 128 to 255, ...) at most 3 rows name the same one
- route_weights: float32 [32768, 2], P(('grp', 'ep', 'tp')), parts along dimension 0, may hold values from 0.1 to 0.9
- w_gate: bfloat16 [128, 2048, 512], P(('ep', 'tp')), may hold values from -0.125 to 0.125
- w_up: bfloat16 [128, 2048, 512], P(('ep', 'tp')), may hold values from -0.125 to 0.125
- w_down: bfloat16 [128, 512, 2048], P(('ep', 'tp')), may hold values from -0.25 to 0.25
Outputs:
- mixed: bfloat16 [32768, 2048], P(('grp', 'ep', 'tp')), parts along dimension 0
The draws below stay inside these ranges and needn't reach their ends.
There are 2 independent parts, one for each index of `grp`. The reference program is written for one: setup_inputs(seed, part) draws one part's arguments, and reference() takes and returns one part's arrays. A program takes and returns all parts, laid end to end along the dimension named above; an argument that names none is the same for every part. Nothing has to cross between parts.
Inputs may be any that keep to these rules, and one draw needn't show every extreme that they name: `route_ids`: each token names 2 different experts. Among the tokens of one device (aligned blocks of 128 tokens) no expert is named more than 3 times, a bound that some block reaches.
All inputs are finite; a program needn't handle non-finite values.
Results may differ from the reference program's by a relative error of at most 0.0071.
Values may be sent and summed in bfloat16 or wider, within the bound.
No kernel may reach another device: no remote copies, remote signals or barrier semaphores. Data moves between devices by JAX's collectives and lax.ppermute only.
A program may use at most 64 MiB of HBM per device.

```python
import math
import jax
import jax.numpy as jnp
import numpy as np
from jax import lax

D = 2048
FF = 512
TOP = 2
TOK_DEV = 128
EXPERTS = 128
CAP = 3
TOKENS = 16384


def block_scale(own_key, shape, shards, least, high):
    loudness, own = 1.0, jax.random.fold_in(own_key, 6)
    for dim, shards_of in shards:
        heights = jnp.exp(jax.random.uniform(jax.random.fold_in(own, dim), (shards_of,), jnp.float32, least / len(shards), high / len(shards)))
        loudness = loudness * jnp.repeat(heights, shape[dim] // shards_of).reshape([-1 if axis == dim else 1 for axis in range(len(shape))])
    return loudness


def routed_block(key, own, number, rows, amount, top, limit, skew):
    order = jax.random.permutation(key, amount)
    packed, ordinary = load_shares(amount, rows * top, limit, skew, True), load_shares(amount, rows * top, limit, skew, False)
    places = jnp.arange(amount)

    def named(lengths, turn):
        used = int((lengths > 0).sum())
        fixed = max(1, used // 4)
        shifted = fixed + (places - fixed + turn * (used - fixed)) % max(1, amount - fixed)
        return jnp.zeros((amount,), jnp.int32).at[order[jnp.where(places < fixed, places, shifted)]].set(jnp.asarray(lengths, jnp.int32))

    lengths = jnp.where(number % 4 == 0, named(packed, number // 4), named(ordinary, number - number // 4 - 1))
    mixed = jax.random.permutation(jax.random.fold_in(own, 3), amount)
    source_of, sink = mixed[0:amount // 2 * 2:2], mixed[1:amount // 2 * 2:2]
    slack = jnp.minimum(lengths[source_of] - 1, limit - lengths[sink]) // 2
    slack = jnp.where((source_of == order[0]) | (sink == order[0]) | (lengths[sink] == 0), 0, jnp.maximum(slack, 0))
    shifted = jax.random.randint(jax.random.fold_in(own, 4), (amount // 2,), 0, 1 << 20) % (slack + 1)
    lengths = lengths.at[source_of].add(-shifted).at[sink].add(shifted)
    labels = jnp.searchsorted(jnp.cumsum(lengths), jnp.arange(rows * top), side="right").astype(jnp.int32)
    table = labels.reshape(top, rows).T
    table = table[jax.random.permutation(jax.random.fold_in(own, 1), rows)]
    turn = jax.random.randint(jax.random.fold_in(own, 2), (rows, 1), 0, top)
    return jnp.take_along_axis(table, (jnp.arange(top)[None, :] + turn) % top, axis=1)


def load_shares(number_of, total, most, lean, full):
    portions = [(1 << 20) // math.isqrt(rank ** lean) + 1 for rank in range(1, number_of + 1)]
    largest = most if full else min(most, max(-(-total // number_of), total * portions[0] // sum(portions)))
    least = 1 if total - largest >= number_of - 1 else 0
    holding, surplus = [largest] + [least] * (number_of - 1), total - largest - least * (number_of - 1)
    while surplus > 0:
        movable = [i for i in range(1, number_of) if holding[i] < largest] or [i for i in range(1, number_of) if holding[i] < most]
        pool, left = sum([portions[i] for i in movable]), surplus
        for i in movable:
            more = min(most - holding[i], max(1, left * portions[i] // pool), surplus)
            holding[i] = holding[i] + more
            surplus = surplus - more
    return np.array(holding)


def centred(stream_key, extent, deviation, most, pieces=(), kind=jnp.bfloat16):
    loudness = block_scale(stream_key, extent, pieces, -0.22, 0.18) if pieces else 1.0
    values = jax.random.normal(stream_key, extent, jnp.float32) * deviation * loudness
    return jnp.minimum(jnp.maximum(values, -most), most).astype(kind)


def setup_inputs(seed: int = 0, part: int = 0) -> dict:
    key_list = jax.random.split(jax.random.key(seed), 8)
    own_keys = jax.random.split(jax.random.fold_in(key_list[7], part), 8)
    tokens = centred(own_keys[0], (TOKENS, D), 1.0, 6.0, ((0, 128),))
    norm_gain = jnp.clip(1.0 + 0.18 * jax.random.normal(key_list[1], (D,), jnp.float32), 0.1, 1.9)
    route_ids_keys = jax.random.split(jax.random.fold_in(own_keys[2], 1), TOKENS // TOK_DEV)
    route_ids_turns = jax.random.permutation(jax.random.fold_in(own_keys[2], 3), TOKENS // TOK_DEV)
    route_ids = jax.vmap(lambda own, number: routed_block(jax.random.fold_in(own_keys[2], 2), own, number, TOK_DEV, EXPERTS, TOP, CAP, 2))(route_ids_keys, route_ids_turns).reshape((TOKENS, TOP))
    route_weights = jnp.clip(0.1 + 0.79999997 * jax.random.uniform(own_keys[3], (TOKENS, TOP), jnp.float32) ** block_scale(own_keys[3], (TOKENS, TOP), ((0, 128),), -0.2, 0.2), 0.1, 0.9)
    w_gate = centred(key_list[4], (EXPERTS, D, FF), D ** -0.5, 0.125, ((0, 128),))
    w_up = centred(key_list[5], (EXPERTS, D, FF), D ** -0.5, 0.125, ((0, 128),))
    w_down = centred(key_list[6], (EXPERTS, FF, D), FF ** -0.5, 0.25, ((0, 128),))
    return {"tokens": tokens, "norm_gain": norm_gain, "route_ids": route_ids, "route_weights": route_weights, "w_gate": w_gate, "w_up": w_up, "w_down": w_down}


def reference(tokens, norm_gain, route_ids, route_weights, w_gate, w_up, w_down):
    source_count = TOKENS // TOK_DEV
    values = tokens.astype(jnp.float32)
    normed = (values * lax.rsqrt(lax.optimization_barrier(jnp.mean(values * values, axis=-1, keepdims=True)) + 1e-06) * norm_gain).astype(jnp.bfloat16)
    per_device = route_ids.reshape(source_count, TOK_DEV * TOP)
    onehot = (per_device[:, :, None] == jnp.arange(EXPERTS, dtype=jnp.int32)[None, None, :]).astype(jnp.int32)
    slot_index = lax.optimization_barrier(jnp.sum((jnp.cumsum(onehot, axis=1) - onehot) * onehot, axis=-1))
    position = (jnp.arange(source_count, dtype=jnp.int32)[:, None] * CAP + slot_index).reshape(-1).astype(jnp.int32)
    flat_ids = route_ids.reshape(-1)
    total_rows = TOKENS * TOP
    row_table = jnp.full((EXPERTS, source_count * CAP), total_rows, jnp.int32)
    row_table = row_table.at[flat_ids, position].set(jnp.arange(total_rows, dtype=jnp.int32))

    def apply_expert(carry, operand):
        table_row, gate_w, up_w, down_w = operand
        token_rows = normed[jnp.minimum(table_row // TOP, TOKENS - 1)]
        gate_act = jnp.dot(token_rows, gate_w, preferred_element_type=jnp.float32)
        up_act = jnp.dot(token_rows, up_w, preferred_element_type=jnp.float32)
        hidden = (jax.nn.silu(gate_act) * up_act).astype(jnp.bfloat16)
        result = jnp.dot(hidden, down_w, preferred_element_type=jnp.float32).astype(jnp.bfloat16)
        return (carry.at[table_row].set(result), None)
    start = jnp.zeros((total_rows + 1, D), jnp.bfloat16)
    picked, _ = lax.scan(apply_expert, start, (row_table, w_gate, w_up, w_down))
    picked = picked[:total_rows].reshape(TOKENS, TOP, D).astype(jnp.float32)
    return lax.optimization_barrier(jnp.sum(picked * route_weights[:, :, None], axis=1)).astype(jnp.bfloat16)
```

```python
import jax
import jax.numpy as jnp
from jax import lax
from jax.sharding import PartitionSpec as P

LANES = 128


def on_device(tokens, norm_gain, route_ids, route_weights, w_gate, w_up, w_down):
    tok_rows, model_width = tokens.shape
    top_count = route_ids.shape[1]
    experts = lax.axis_size("ep") * lax.axis_size("tp")
    capacity = 3 * tok_rows * top_count // (2 * experts)
    values = tokens.astype(jnp.float32)
    normed = (
        values * lax.rsqrt(jnp.mean(values * values, axis=-1, keepdims=True) + 1e-06) * norm_gain
    ).astype(jnp.bfloat16)
    experts_iota = jnp.arange(experts, dtype=jnp.int32)[:, None]
    ids = route_ids.T
    picks = [ids[k][None, :] == experts_iota for k in range(top_count)]
    named = picks[0]
    for pick in picks[1:]:
        named = named | pick
    earlier = jnp.triu(jnp.ones((tok_rows, tok_rows), jnp.bfloat16), 1)
    rank = jnp.dot(named.astype(jnp.bfloat16), earlier, preferred_element_type=jnp.float32)
    slots = jnp.arange(capacity, dtype=jnp.float32)[None, :, None]
    in_slot = rank[:, None, :] == slots

    def table(mask):
        chosen = (mask[:, None, :] & in_slot).astype(jnp.bfloat16)
        return chosen.reshape(experts * capacity, tok_rows)

    sent = jnp.dot(table(named), normed, preferred_element_type=jnp.float32).astype(jnp.bfloat16)

    def exchange(rows):
        blocks = rows.reshape(experts, capacity * model_width // LANES, LANES)
        moved = lax.all_to_all(blocks, ("ep", "tp"), split_axis=0, concat_axis=0, tiled=True)
        return moved.reshape(experts * capacity, model_width)

    flat_rows = exchange(sent)
    gate_act = jnp.dot(flat_rows, w_gate[0], preferred_element_type=jnp.float32)
    up_act = jnp.dot(flat_rows, w_up[0], preferred_element_type=jnp.float32)
    hidden = (jax.nn.silu(gate_act) * up_act).astype(jnp.bfloat16)
    result = jnp.dot(hidden, w_down[0], preferred_element_type=jnp.float32).astype(jnp.bfloat16)
    returned = exchange(result)
    mixed = jnp.zeros((tok_rows, model_width), jnp.float32)
    for k in range(top_count):
        picked = lax.dot_general(
            table(picks[k]), returned, (((0,), (0,)), ((), ())), preferred_element_type=jnp.float32
        )
        mixed = mixed + picked * route_weights[:, k : k + 1]
    return mixed.astype(jnp.bfloat16)


def solution(mesh):
    return jax.shard_map(
        on_device,
        mesh=mesh,
        in_specs=(
            P(("grp", "ep", "tp"), None),
            P(),
            P(("grp", "ep", "tp"), None),
            P(("grp", "ep", "tp"), None),
            P(("ep", "tp"), None, None),
            P(("ep", "tp"), None, None),
            P(("ep", "tp"), None, None),
        ),
        out_specs=P(("grp", "ep", "tp"), None),
        check_vma=False,
    )
```

```python
import jax
import jax.numpy as jnp
from jax import lax
from jax.sharding import PartitionSpec as P

AXES = ("ep", "tp")
CORES = 2


def on_device(tokens, norm_gain, route_ids, route_weights, w_gate, w_up, w_down):
    tok_rows, model_width = tokens.shape
    top_count = route_ids.shape[1]
    columns = CORES * lax.axis_size("tp")
    planes = lax.axis_size("ep") // CORES
    experts = planes * columns
    capacity = 3 * tok_rows * top_count // (2 * experts)
    block = columns * capacity
    plane = lax.axis_index("ep") // CORES

    shifts = [d if d <= planes // 2 else d - planes for d in range(planes)]
    chunks = [[d for d in shifts if d % 2 == 0], [d for d in shifts if d % 2]]

    def move(rows, hop):
        pairs = [
            (p * columns + j, (p + hop) % planes * columns + j)
            for p in range(planes)
            for j in range(columns)
        ]
        return lax.ppermute(rows, AXES, pairs)

    def along_z(blocks, sign):
        here, left = {}, {}
        for d, rows in blocks.items():
            if d == 0:
                here[d] = rows
            elif abs(d) == planes // 2:
                here[d] = ("direct", rows)
            else:
                left[d] = [rows, sign * d]
        hop = planes // 4
        first = True
        while hop:
            for way in (1, -1):
                moved = [d for d, (_, rest) in left.items() if rest * way > 0 and abs(rest) & hop]
                if not moved:
                    continue
                rows = [left[d][0] for d in moved]
                got = move(jnp.concatenate(rows, 0) if len(rows) > 1 else rows[0], way * hop)
                for i, d in enumerate(moved):
                    left[d] = [got[i * block : (i + 1) * block], left[d][1] - way * hop]
            if first:
                for d, v in here.items():
                    if isinstance(v, tuple):
                        here[d] = move(v[1], d)
                first = False
            hop //= 2
        for d, (rows, _) in left.items():
            here[d] = rows
        return here

    groups = [[p * columns + j for j in range(columns)] for p in range(planes)]

    def in_plane(rows):
        parts = rows.reshape(columns, -1, model_width)
        moved = lax.all_to_all(
            parts, AXES, split_axis=0, concat_axis=0, axis_index_groups=groups, tiled=True
        )
        return moved.reshape(-1, model_width)

    def regroup(rows, outer, inner):
        r = jnp.arange(outer * inner * capacity, dtype=jnp.int32)
        i, rest = r // (outer * capacity), r % (outer * capacity)
        o, s = rest // capacity, rest % capacity
        source = (o * inner + i) * capacity + s
        table = (source[:, None] == r[None, :]).astype(jnp.bfloat16)
        return jnp.dot(table, rows, preferred_element_type=jnp.float32).astype(jnp.bfloat16)

    values = tokens.astype(jnp.float32)
    normed = (
        values * lax.rsqrt(jnp.mean(values * values, axis=-1, keepdims=True) + 1e-06) * norm_gain
    ).astype(jnp.bfloat16)
    ids = route_ids.T
    earlier = jnp.triu(jnp.ones((tok_rows, tok_rows), jnp.bfloat16), 1)

    def tables(chunk):
        r = jnp.arange(block * len(chunk), dtype=jnp.int32)
        shift = jnp.asarray(chunk, jnp.int32)[:, None] + jnp.zeros((1, block), jnp.int32)
        expert = (plane + shift.reshape(-1) + planes) % planes * columns + r % block // capacity
        picks = [ids[k][None, :] == expert[:, None] for k in range(top_count)]
        named = picks[0]
        for pick in picks[1:]:
            named = named | pick
        rank = jnp.dot(named.astype(jnp.bfloat16), earlier, preferred_element_type=jnp.float32)
        in_slot = rank == (r % capacity).astype(jnp.float32)[:, None]
        sent = (named & in_slot).astype(jnp.bfloat16)
        return sent, [(pick & in_slot).astype(jnp.bfloat16) for pick in picks]

    def products(rows):
        gate_act = jnp.dot(rows, w_gate[0], preferred_element_type=jnp.float32)
        up_act = jnp.dot(rows, w_up[0], preferred_element_type=jnp.float32)
        hidden = (jax.nn.silu(gate_act) * up_act).astype(jnp.bfloat16)
        return jnp.dot(hidden, w_down[0], preferred_element_type=jnp.float32).astype(jnp.bfloat16)

    made = []
    for chunk in chunks:
        sent_table, pick_tables = tables(chunk)
        rows = jnp.dot(sent_table, normed, preferred_element_type=jnp.float32).astype(jnp.bfloat16)
        made.append((rows, pick_tables))

    mixed = jnp.zeros((tok_rows, model_width), jnp.float32)
    parts = [mixed] * top_count
    for chunk, (rows, pick_tables) in zip(chunks, made):
        blocks = {d: rows[i * block : (i + 1) * block] for i, d in enumerate(chunk)}
        arrived = along_z(blocks, 1)
        rows = jnp.concatenate([arrived[d] for d in chunk], 0)
        rows = in_plane(regroup(rows, len(chunk), columns))
        rows = in_plane(products(rows))
        rows = regroup(rows, columns, len(chunk))
        blocks = {d: rows[i * block : (i + 1) * block] for i, d in enumerate(chunk)}
        arrived = along_z(blocks, -1)
        rows = jnp.concatenate([arrived[d] for d in chunk], 0)
        for k in range(top_count):
            parts[k] = parts[k] + lax.dot_general(
                pick_tables[k], rows, (((0,), (0,)), ((), ())), preferred_element_type=jnp.float32
            )
    for k in range(top_count):
        mixed = mixed + parts[k] * route_weights[:, k : k + 1]
    return mixed.astype(jnp.bfloat16)


def solution(mesh):
    return jax.shard_map(
        on_device,
        mesh=mesh,
        in_specs=(
            P(("grp", "ep", "tp"), None),
            P(),
            P(("grp", "ep", "tp"), None),
            P(("grp", "ep", "tp"), None),
            P(("ep", "tp"), None, None),
            P(("ep", "tp"), None, None),
            P(("ep", "tp"), None, None),
        ),
        out_specs=P(("grp", "ep", "tp"), None),
        check_vma=False,
    )
```

```python
import jax
import jax.numpy as jnp
from jax import lax
from jax.experimental import pallas as pl
from jax.experimental.pallas import tpu as pltpu
from jax.sharding import PartitionSpec as P

LANES = 128
AXES = ("ep", "tp")
MIB = 1 << 20
WHOLE = pl.BlockSpec(memory_space=pltpu.VMEM)


def swap_table(tiles):
    n = tiles * tiles
    row = lax.broadcasted_iota(jnp.int32, (n, n), 0)
    column = lax.broadcasted_iota(jnp.int32, (n, n), 1)
    source = lax.rem(row, tiles) * tiles + lax.div(row, tiles)
    return (column == source).astype(jnp.bfloat16)


def spread_rows(table, rows_ref, out_ref):
    n, width = rows_ref.shape
    tiles = width // LANES
    span = tiles * tiles
    for g in range(0, n, 2 * tiles):
        halves = []
        for h in (g, g + tiles):
            pieces = [rows_ref[h : h + tiles, c * LANES : (c + 1) * LANES] for c in range(tiles)]
            halves.append(jnp.concatenate(pieces, 0))
        both = jnp.dot(table, jnp.concatenate(halves, 1), preferred_element_type=jnp.float32)
        both = both.astype(jnp.bfloat16)
        out_ref[g * tiles : g * tiles + span, :] = both[:, :LANES]
        out_ref[g * tiles + span : g * tiles + 2 * span, :] = both[:, LANES:]


def gather_rows(table, in_ref, rows_ref):
    n, width = rows_ref.shape
    tiles = width // LANES
    span = tiles * tiles
    for g in range(0, n, 2 * tiles):
        first = in_ref[g * tiles : g * tiles + span, :]
        second = in_ref[g * tiles + span : g * tiles + 2 * span, :]
        both = jnp.dot(
            table, jnp.concatenate([first, second], 1), preferred_element_type=jnp.float32
        ).astype(jnp.bfloat16)
        for c in range(tiles):
            part = both[c * tiles : (c + 1) * tiles]
            rows_ref[g : g + tiles, c * LANES : (c + 1) * LANES] = part[:, :LANES]
            rows_ref[g + tiles : g + 2 * tiles, c * LANES : (c + 1) * LANES] = part[:, LANES:]


def dispatch_kernel(capacity, tokens_ref, gain_ref, ids_ref, out_ref, rows_ref):
    tok_rows, width = tokens_ref.shape
    top_count = ids_ref.shape[0]
    n = rows_ref.shape[0]
    values = tokens_ref[...].astype(jnp.float32)
    scale = lax.rsqrt(jnp.mean(values * values, axis=-1, keepdims=True) + 1e-06)
    normed = (values * scale * gain_ref[...]).astype(jnp.bfloat16)
    row = lax.broadcasted_iota(jnp.int32, (n, tok_rows), 0)
    expert = lax.div(row, capacity)
    named = ids_ref[0:1, :] == expert
    for k in range(1, top_count):
        named = named | (ids_ref[k : k + 1, :] == expert)
    before = lax.broadcasted_iota(jnp.int32, (tok_rows, tok_rows), 0)
    after = lax.broadcasted_iota(jnp.int32, (tok_rows, tok_rows), 1)
    earlier = (before < after).astype(jnp.bfloat16)
    rank = jnp.dot(named.astype(jnp.bfloat16), earlier, preferred_element_type=jnp.float32)
    slot = lax.rem(row, capacity).astype(jnp.float32)
    table = (named & (rank == slot)).astype(jnp.bfloat16)
    rows_ref[...] = jnp.dot(table, normed, preferred_element_type=jnp.float32).astype(jnp.bfloat16)
    spread_rows(swap_table(width // LANES), rows_ref, out_ref)


def picks_kernel(capacity, ids_ref, *out_refs):
    tok_rows = ids_ref.shape[0]
    n = out_refs[0].shape[1]
    row = lax.broadcasted_iota(jnp.int32, (tok_rows, n), 1)
    expert = lax.div(row, capacity)
    picks = [ids_ref[:, k : k + 1] == expert for k in range(len(out_refs))]
    named = picks[0]
    for pick in picks[1:]:
        named = named | pick
    after = lax.broadcasted_iota(jnp.int32, (tok_rows, tok_rows), 0)
    before = lax.broadcasted_iota(jnp.int32, (tok_rows, tok_rows), 1)
    earlier = (before < after).astype(jnp.bfloat16)
    rank = jnp.dot(earlier, named.astype(jnp.bfloat16), preferred_element_type=jnp.float32)
    in_slot = rank == lax.rem(row, capacity).astype(jnp.float32)
    for pick, out_ref in zip(picks, out_refs):
        out_ref[...] = (pick & in_slot).astype(jnp.bfloat16)


def products_kernel(in_ref, gate_ref, up_ref, down_ref, out_ref, rows_ref, hidden_ref):
    width, hidden_width = gate_ref.shape
    table = swap_table(width // LANES)
    gather_rows(table, in_ref, rows_ref)
    rows = rows_ref[...]
    step = 256
    for f in range(0, hidden_width, step):
        gate_act = jnp.dot(rows, gate_ref[:, f : f + step], preferred_element_type=jnp.float32)
        up_act = jnp.dot(rows, up_ref[:, f : f + step], preferred_element_type=jnp.float32)
        hidden_ref[:, f : f + step] = (jax.nn.silu(gate_act) * up_act).astype(jnp.bfloat16)
    hidden = hidden_ref[...]
    for d in range(0, width, step):
        part = jnp.dot(hidden, down_ref[:, d : d + step], preferred_element_type=jnp.float32)
        rows_ref[:, d : d + step] = part.astype(jnp.bfloat16)
    spread_rows(table, rows_ref, out_ref)


def mix_kernel(in_ref, weights_ref, *refs):
    *pick_refs, out_ref, rows_ref = refs
    width = out_ref.shape[1]
    gather_rows(swap_table(width // LANES), in_ref, rows_ref)
    step = 512
    for d in range(0, width, step):
        total = None
        for k, pick_ref in enumerate(pick_refs):
            picked = jnp.dot(
                pick_ref[...], rows_ref[:, d : d + step], preferred_element_type=jnp.float32
            )
            term = picked * weights_ref[:, k : k + 1]
            total = term if total is None else total + term
        out_ref[:, d : d + step] = total.astype(out_ref.dtype)


def on_device(tokens, norm_gain, route_ids, route_weights, w_gate, w_up, w_down):
    tok_rows, width = tokens.shape
    top_count = route_ids.shape[1]
    hidden_width = w_gate.shape[2]
    experts = lax.axis_size("ep") * lax.axis_size("tp")
    capacity = 3 * tok_rows * top_count // (2 * experts)
    n = experts * capacity
    tiles = width // LANES
    flat = jax.ShapeDtypeStruct((n * tiles, LANES), jnp.bfloat16)
    rows_scratch = pltpu.VMEM((n, width), jnp.bfloat16)

    def call(kernel, out_shape, inputs, scratch, name, flops, mib):
        many = isinstance(out_shape, (list, tuple))
        return pl.pallas_call(
            kernel,
            out_shape=out_shape,
            in_specs=[WHOLE] * len(inputs),
            out_specs=[WHOLE] * len(out_shape) if many else WHOLE,
            scratch_shapes=scratch,
            name=name,
            cost_estimate=pl.CostEstimate(flops=flops, bytes_accessed=4 * MIB, transcendentals=0),
            compiler_params=pltpu.CompilerParams(vmem_limit_bytes=mib * MIB),
        )(*inputs)

    def exchange(rows):
        blocks = rows.reshape(experts, capacity * tiles, LANES)
        moved = lax.all_to_all(blocks, AXES, split_axis=0, concat_axis=0, tiled=True)
        return moved.reshape(n * tiles, LANES)

    sent = call(
        lambda *refs: dispatch_kernel(capacity, *refs),
        flat,
        [tokens, norm_gain.reshape(1, width), route_ids.T],
        [rows_scratch],
        "dispatch",
        2 * n * tok_rows * width,
        20,
    )
    received = exchange(sent)
    pick_shape = jax.ShapeDtypeStruct((tok_rows, n), jnp.bfloat16)
    picks = call(
        lambda *refs: picks_kernel(capacity, *refs),
        [pick_shape] * top_count,
        [route_ids],
        [],
        "picks",
        2 * n * tok_rows * tok_rows,
        8,
    )
    result = call(
        products_kernel,
        flat,
        [received, w_gate[0], w_up[0], w_down[0]],
        [rows_scratch, pltpu.VMEM((n, hidden_width), jnp.bfloat16)],
        "products",
        6 * n * width * hidden_width,
        28,
    )
    returned = exchange(result)
    return call(
        mix_kernel,
        jax.ShapeDtypeStruct(tokens.shape, tokens.dtype),
        [returned, route_weights, *picks],
        [rows_scratch],
        "mix",
        2 * top_count * n * tok_rows * width,
        20,
    )


def solution(mesh):
    return jax.shard_map(
        on_device,
        mesh=mesh,
        in_specs=(
            P(("grp", "ep", "tp"), None),
            P(),
            P(("grp", "ep", "tp"), None),
            P(("grp", "ep", "tp"), None),
            P(("ep", "tp"), None, None),
            P(("ep", "tp"), None, None),
            P(("ep", "tp"), None, None),
        ),
        out_specs=P(("grp", "ep", "tp"), None),
        check_vma=False,
    )
```

```python
import jax
import jax.numpy as jnp
from jax import lax
from jax.experimental import pallas as pl
from jax.experimental.pallas import tpu as pltpu
from jax.sharding import PartitionSpec as P

LANES = 128
AXES = ("ep", "tp")
MIB = 1 << 20
WHOLE = pl.BlockSpec(memory_space=pltpu.VMEM)
OUTSIDE = pl.BlockSpec(memory_space=pltpu.HBM)


def swap_table(tiles):
    n = tiles * tiles
    row = lax.broadcasted_iota(jnp.int32, (n, n), 0)
    column = lax.broadcasted_iota(jnp.int32, (n, n), 1)
    source = lax.rem(row, tiles) * tiles + lax.div(row, tiles)
    return (column == source).astype(jnp.bfloat16)


def spread_rows(table, rows_ref, out_ref, done=None, parts=1):
    n, width = rows_ref.shape
    tiles = width // LANES
    span = tiles * tiles
    for g in range(0, n, 2 * tiles):
        halves = []
        for h in (g, g + tiles):
            pieces = [rows_ref[h : h + tiles, c * LANES : (c + 1) * LANES] for c in range(tiles)]
            halves.append(jnp.concatenate(pieces, 0))
        both = jnp.dot(table, jnp.concatenate(halves, 1), preferred_element_type=jnp.float32)
        both = both.astype(jnp.bfloat16)
        out_ref[g * tiles : g * tiles + span, :] = both[:, :LANES]
        out_ref[g * tiles + span : g * tiles + 2 * span, :] = both[:, LANES:]
        part = n // parts
        if done is not None and (g + 2 * tiles) % part == 0:
            done((g + 2 * tiles - part) * tiles, (g + 2 * tiles) * tiles)


def gather_rows(table, in_ref, rows_ref):
    n, width = rows_ref.shape
    tiles = width // LANES
    span = tiles * tiles
    for g in range(0, n, 2 * tiles):
        first = in_ref[g * tiles : g * tiles + span, :]
        second = in_ref[g * tiles + span : g * tiles + 2 * span, :]
        both = jnp.dot(
            table, jnp.concatenate([first, second], 1), preferred_element_type=jnp.float32
        ).astype(jnp.bfloat16)
        for c in range(tiles):
            part = both[c * tiles : (c + 1) * tiles]
            rows_ref[g : g + tiles, c * LANES : (c + 1) * LANES] = part[:, :LANES]
            rows_ref[g + tiles : g + 2 * tiles, c * LANES : (c + 1) * LANES] = part[:, LANES:]


def dispatch_kernel(capacity, tokens_ref, gain_ref, ids_ref, rows_ref):
    tok_rows, width = tokens_ref.shape
    top_count = ids_ref.shape[0]
    n = rows_ref.shape[0]
    values = tokens_ref[...].astype(jnp.float32)
    scale = lax.rsqrt(jnp.mean(values * values, axis=-1, keepdims=True) + 1e-06)
    normed = (values * scale * gain_ref[...]).astype(jnp.bfloat16)
    row = lax.broadcasted_iota(jnp.int32, (n, tok_rows), 0)
    expert = lax.div(row, capacity)
    named = ids_ref[0:1, :] == expert
    for k in range(1, top_count):
        named = named | (ids_ref[k : k + 1, :] == expert)
    before = lax.broadcasted_iota(jnp.int32, (tok_rows, tok_rows), 0)
    after = lax.broadcasted_iota(jnp.int32, (tok_rows, tok_rows), 1)
    earlier = (before < after).astype(jnp.bfloat16)
    rank = jnp.dot(named.astype(jnp.bfloat16), earlier, preferred_element_type=jnp.float32)
    slot = lax.rem(row, capacity).astype(jnp.float32)
    table = (named & (rank == slot)).astype(jnp.bfloat16)
    rows_ref[...] = jnp.dot(table, normed, preferred_element_type=jnp.float32).astype(jnp.bfloat16)


def spread_kernel(rows_ref, out_ref):
    spread_rows(swap_table(rows_ref.shape[1] // LANES), rows_ref, out_ref)


def picks_kernel(capacity, ids_ref, *out_refs):
    tok_rows = ids_ref.shape[0]
    n = out_refs[0].shape[1]
    row = lax.broadcasted_iota(jnp.int32, (tok_rows, n), 1)
    expert = lax.div(row, capacity)
    picks = [ids_ref[:, k : k + 1] == expert for k in range(len(out_refs))]
    named = picks[0]
    for pick in picks[1:]:
        named = named | pick
    after = lax.broadcasted_iota(jnp.int32, (tok_rows, tok_rows), 0)
    before = lax.broadcasted_iota(jnp.int32, (tok_rows, tok_rows), 1)
    earlier = (before < after).astype(jnp.bfloat16)
    rank = jnp.dot(earlier, named.astype(jnp.bfloat16), preferred_element_type=jnp.float32)
    in_slot = rank == lax.rem(row, capacity).astype(jnp.float32)
    for pick, out_ref in zip(picks, out_refs):
        out_ref[...] = (pick & in_slot).astype(jnp.bfloat16)


def products_kernel(
    in_ref, gate_ref, up_ref, down_ref, out_hbm, rows_ref, hidden_ref, out_ref, sems
):
    width, hidden_width = gate_ref.shape
    table = swap_table(width // LANES)
    gather_rows(table, in_ref, rows_ref)
    rows = rows_ref[...]
    step = 256
    for f in range(0, hidden_width, step):
        gate_act = jnp.dot(rows, gate_ref[:, f : f + step], preferred_element_type=jnp.float32)
        up_act = jnp.dot(rows, up_ref[:, f : f + step], preferred_element_type=jnp.float32)
        hidden_ref[:, f : f + step] = (jax.nn.silu(gate_act) * up_act).astype(jnp.bfloat16)
    hidden = hidden_ref[...]
    for d in range(0, width, step):
        part = jnp.dot(hidden, down_ref[:, d : d + step], preferred_element_type=jnp.float32)
        rows_ref[:, d : d + step] = part.astype(jnp.bfloat16)
    copies = []

    def send(first, last):
        part = slice(first, last)
        copy = pltpu.make_async_copy(out_ref.at[part], out_hbm.at[part], sems.at[len(copies)])
        copy.start()
        copies.append(copy)

    spread_rows(table, rows_ref, out_ref, send, sems.shape[0])
    for copy in copies:
        copy.wait()


def mix_kernel(in_ref, weights_ref, *refs):
    *pick_refs, out_hbm, rows_ref, mixed_ref, sems = refs
    width = mixed_ref.shape[1]
    gather_rows(swap_table(width // LANES), in_ref, rows_ref)
    step = width // sems.shape[0]
    copies = []
    for i in range(sems.shape[0]):
        columns = slice(i * step, (i + 1) * step)
        total = None
        for k, pick_ref in enumerate(pick_refs):
            picked = jnp.dot(
                pick_ref[...], rows_ref[:, columns], preferred_element_type=jnp.float32
            )
            term = picked * weights_ref[:, k : k + 1]
            total = term if total is None else total + term
        mixed_ref[:, columns] = total.astype(mixed_ref.dtype)
        copy = pltpu.make_async_copy(mixed_ref.at[:, columns], out_hbm.at[:, columns], sems.at[i])
        copy.start()
        copies.append(copy)
    for copy in copies:
        copy.wait()


def on_device(tokens, norm_gain, route_ids, route_weights, w_gate, w_up, w_down):
    tok_rows, width = tokens.shape
    top_count = route_ids.shape[1]
    hidden_width = w_gate.shape[2]
    experts = lax.axis_size("ep") * lax.axis_size("tp")
    capacity = 3 * tok_rows * top_count // (2 * experts)
    n = experts * capacity
    tiles = width // LANES
    flat = jax.ShapeDtypeStruct((n * tiles, LANES), jnp.bfloat16)
    rows_scratch = pltpu.VMEM((n, width), jnp.bfloat16)

    def call(kernel, out_shape, inputs, scratch, name, flops, mib, outside=(), out_spec=WHOLE):
        many = isinstance(out_shape, (list, tuple))
        return pl.pallas_call(
            kernel,
            out_shape=out_shape,
            in_specs=[OUTSIDE if i in outside else WHOLE for i in range(len(inputs))],
            out_specs=[out_spec] * len(out_shape) if many else out_spec,
            scratch_shapes=scratch,
            name=name,
            cost_estimate=pl.CostEstimate(flops=flops, bytes_accessed=4 * MIB, transcendentals=0),
            compiler_params=pltpu.CompilerParams(vmem_limit_bytes=mib * MIB),
        )(*inputs)

    def exchange(rows):
        blocks = rows.reshape(experts, capacity * tiles, LANES)
        moved = lax.all_to_all(blocks, AXES, split_axis=0, concat_axis=0, tiled=True)
        return moved.reshape(n * tiles, LANES)

    rows = call(
        lambda *refs: dispatch_kernel(capacity, *refs),
        jax.ShapeDtypeStruct((n, width), jnp.bfloat16),
        [tokens, norm_gain.reshape(1, width), route_ids.T],
        [],
        "dispatch",
        2 * n * tok_rows * width,
        16,
    )
    sent = call(spread_kernel, flat, [rows], [], "spread", 2 * n * 256 * width, 16)
    received = exchange(sent)
    pick_shape = jax.ShapeDtypeStruct((tok_rows, n), jnp.bfloat16)
    picks = call(
        lambda *refs: picks_kernel(capacity, *refs),
        [pick_shape] * top_count,
        [route_ids],
        [],
        "picks",
        2 * n * tok_rows * tok_rows,
        8,
    )
    result = call(
        products_kernel,
        flat,
        [received, w_gate[0], w_up[0], w_down[0]],
        [
            rows_scratch,
            pltpu.VMEM((n, hidden_width), jnp.bfloat16),
            pltpu.VMEM(flat.shape, flat.dtype),
            pltpu.SemaphoreType.DMA((4,)),
        ],
        "products",
        6 * n * width * hidden_width,
        28,
        out_spec=OUTSIDE,
    )
    returned = exchange(result)
    return call(
        mix_kernel,
        jax.ShapeDtypeStruct(tokens.shape, tokens.dtype),
        [returned, route_weights, *picks],
        [
            rows_scratch,
            pltpu.VMEM(tokens.shape, tokens.dtype),
            pltpu.SemaphoreType.DMA((4,)),
        ],
        "mix",
        2 * top_count * n * tok_rows * width,
        20,
        out_spec=OUTSIDE,
    )


def solution(mesh):
    return jax.shard_map(
        on_device,
        mesh=mesh,
        in_specs=(
            P(("grp", "ep", "tp"), None),
            P(),
            P(("grp", "ep", "tp"), None),
            P(("grp", "ep", "tp"), None),
            P(("ep", "tp"), None, None),
            P(("ep", "tp"), None, None),
            P(("ep", "tp"), None, None),
        ),
        out_specs=P(("grp", "ep", "tp"), None),
        check_vma=False,
    )
```

```python
import jax
import jax.numpy as jnp
from jax import lax
from jax.experimental import pallas as pl
from jax.experimental.pallas import tpu as pltpu
from jax.sharding import PartitionSpec as P

LANES = 128
AXES = ("ep", "tp")
MIB = 1 << 20
AHEAD = 1 << 32
WHOLE = pl.BlockSpec(memory_space=pltpu.VMEM)
OUTSIDE = pl.BlockSpec(memory_space=pltpu.HBM)


def swap_kernel(tiles, out_ref):
    n = tiles * tiles
    row = lax.broadcasted_iota(jnp.int32, (n, n), 0)
    column = lax.broadcasted_iota(jnp.int32, (n, n), 1)
    source = lax.rem(row, tiles) * tiles + lax.div(row, tiles)
    out_ref[...] = (column == source).astype(jnp.bfloat16)


def spread_rows(table, rows_ref, out_ref, done=None, parts=1):
    n, width = rows_ref.shape
    tiles = width // LANES
    span = tiles * tiles
    for g in range(0, n, 2 * tiles):
        halves = []
        for h in (g, g + tiles):
            pieces = [rows_ref[h : h + tiles, c * LANES : (c + 1) * LANES] for c in range(tiles)]
            halves.append(jnp.concatenate(pieces, 0))
        both = jnp.dot(table, jnp.concatenate(halves, 1), preferred_element_type=jnp.float32)
        both = both.astype(jnp.bfloat16)
        out_ref[g * tiles : g * tiles + span, :] = both[:, :LANES]
        out_ref[g * tiles + span : g * tiles + 2 * span, :] = both[:, LANES:]
        part = n // parts
        if done is not None and (g + 2 * tiles) % part == 0:
            done((g + 2 * tiles - part) * tiles, (g + 2 * tiles) * tiles)


def gather_rows(table, in_ref, rows_ref):
    n, width = rows_ref.shape
    tiles = width // LANES
    span = tiles * tiles
    for g in range(0, n, 2 * tiles):
        first = in_ref[g * tiles : g * tiles + span, :]
        second = in_ref[g * tiles + span : g * tiles + 2 * span, :]
        both = jnp.dot(
            table, jnp.concatenate([first, second], 1), preferred_element_type=jnp.float32
        ).astype(jnp.bfloat16)
        for c in range(tiles):
            part = both[c * tiles : (c + 1) * tiles]
            rows_ref[g : g + tiles, c * LANES : (c + 1) * LANES] = part[:, :LANES]
            rows_ref[g + tiles : g + 2 * tiles, c * LANES : (c + 1) * LANES] = part[:, LANES:]


def table_kernel(capacity, ids_ref, table_ref):
    n, tok_rows = table_ref.shape
    row = lax.broadcasted_iota(jnp.int32, (n, tok_rows), 0)
    expert = lax.div(row, capacity)
    named = ids_ref[0:1, :] == expert
    for k in range(1, ids_ref.shape[0]):
        named = named | (ids_ref[k : k + 1, :] == expert)
    before = lax.broadcasted_iota(jnp.int32, (tok_rows, tok_rows), 0)
    after = lax.broadcasted_iota(jnp.int32, (tok_rows, tok_rows), 1)
    earlier = (before < after).astype(jnp.bfloat16)
    rank = jnp.dot(named.astype(jnp.bfloat16), earlier, preferred_element_type=jnp.float32)
    slot = lax.rem(row, capacity).astype(jnp.float32)
    table_ref[...] = (named & (rank == slot)).astype(jnp.bfloat16)


def dispatch_kernel(tokens_ref, gain_ref, table_ref, rows_ref):
    values = tokens_ref[...].astype(jnp.float32)
    scale = lax.rsqrt(jnp.mean(values * values, axis=-1, keepdims=True) + 1e-06)
    normed = (values * scale * gain_ref[...]).astype(jnp.bfloat16)
    rows = jnp.dot(table_ref[...], normed, preferred_element_type=jnp.float32)
    rows_ref[...] = rows.astype(jnp.bfloat16)


def spread_kernel(swap_ref, rows_ref, out_ref):
    spread_rows(swap_ref[...], rows_ref, out_ref)


def picks_kernel(capacity, ids_ref, *out_refs):
    tok_rows = ids_ref.shape[0]
    n = out_refs[0].shape[1]
    row = lax.broadcasted_iota(jnp.int32, (tok_rows, n), 1)
    expert = lax.div(row, capacity)
    picks = [ids_ref[:, k : k + 1] == expert for k in range(len(out_refs))]
    named = picks[0]
    for pick in picks[1:]:
        named = named | pick
    after = lax.broadcasted_iota(jnp.int32, (tok_rows, tok_rows), 0)
    before = lax.broadcasted_iota(jnp.int32, (tok_rows, tok_rows), 1)
    earlier = (before < after).astype(jnp.bfloat16)
    rank = jnp.dot(earlier, named.astype(jnp.bfloat16), preferred_element_type=jnp.float32)
    in_slot = rank == lax.rem(row, capacity).astype(jnp.float32)
    for pick, out_ref in zip(picks, out_refs):
        out_ref[...] = (pick & in_slot).astype(jnp.bfloat16)


def products_kernel(
    swap_ref, in_ref, gate_ref, up_ref, down_ref, out_hbm, rows_ref, hidden_ref, out_ref, sems
):
    width, hidden_width = gate_ref.shape
    table = swap_ref[...]
    gather_rows(table, in_ref, rows_ref)
    rows = rows_ref[...]
    step = 256
    for f in range(0, hidden_width, step):
        gate_act = jnp.dot(rows, gate_ref[:, f : f + step], preferred_element_type=jnp.float32)
        up_act = jnp.dot(rows, up_ref[:, f : f + step], preferred_element_type=jnp.float32)
        hidden_ref[:, f : f + step] = (jax.nn.silu(gate_act) * up_act).astype(jnp.bfloat16)
    hidden = hidden_ref[...]
    for d in range(0, width, step):
        part = jnp.dot(hidden, down_ref[:, d : d + step], preferred_element_type=jnp.float32)
        rows_ref[:, d : d + step] = part.astype(jnp.bfloat16)
    copies = []

    def send(first, last):
        part = slice(first, last)
        copy = pltpu.make_async_copy(out_ref.at[part], out_hbm.at[part], sems.at[len(copies)])
        copy.start()
        copies.append(copy)

    spread_rows(table, rows_ref, out_ref, send, sems.shape[0])
    for copy in copies:
        copy.wait()


def mix_kernel(swap_ref, in_ref, weights_ref, *refs):
    *pick_refs, out_hbm, rows_ref, mixed_ref, sems = refs
    width = mixed_ref.shape[1]
    gather_rows(swap_ref[...], in_ref, rows_ref)
    step = width // sems.shape[0]
    copies = []
    for i in range(sems.shape[0]):
        columns = slice(i * step, (i + 1) * step)
        total = None
        for k, pick_ref in enumerate(pick_refs):
            picked = jnp.dot(
                pick_ref[...], rows_ref[:, columns], preferred_element_type=jnp.float32
            )
            term = picked * weights_ref[:, k : k + 1]
            total = term if total is None else total + term
        mixed_ref[:, columns] = total.astype(mixed_ref.dtype)
        copy = pltpu.make_async_copy(mixed_ref.at[:, columns], out_hbm.at[:, columns], sems.at[i])
        copy.start()
        copies.append(copy)
    for copy in copies:
        copy.wait()


def on_device(tokens, norm_gain, route_ids, route_weights, w_gate, w_up, w_down):
    tok_rows, width = tokens.shape
    top_count = route_ids.shape[1]
    hidden_width = w_gate.shape[2]
    experts = lax.axis_size("ep") * lax.axis_size("tp")
    capacity = 3 * tok_rows * top_count // (2 * experts)
    n = experts * capacity
    tiles = width // LANES
    flat = jax.ShapeDtypeStruct((n * tiles, LANES), jnp.bfloat16)
    rows_scratch = pltpu.VMEM((n, width), jnp.bfloat16)

    def call(kernel, out_shape, inputs, scratch, name, flops, mib, outside=(), out_spec=WHOLE):
        many = isinstance(out_shape, (list, tuple))
        return pl.pallas_call(
            kernel,
            out_shape=out_shape,
            in_specs=[OUTSIDE if i in outside else WHOLE for i in range(len(inputs))],
            out_specs=[out_spec] * len(out_shape) if many else out_spec,
            scratch_shapes=scratch,
            name=name,
            cost_estimate=pl.CostEstimate(flops=flops, bytes_accessed=4 * MIB, transcendentals=0),
            compiler_params=pltpu.CompilerParams(vmem_limit_bytes=mib * MIB),
        )(*inputs)

    def exchange(rows):
        blocks = rows.reshape(experts, capacity * tiles, LANES)
        moved = lax.all_to_all(blocks, AXES, split_axis=0, concat_axis=0, tiled=True)
        return moved.reshape(n * tiles, LANES)

    swap = call(
        lambda ref: swap_kernel(tiles, ref),
        jax.ShapeDtypeStruct((tiles * tiles, tiles * tiles), jnp.bfloat16),
        [],
        [],
        "swap",
        AHEAD,
        4,
    )
    table = call(
        lambda *refs: table_kernel(capacity, *refs),
        jax.ShapeDtypeStruct((n, tok_rows), jnp.bfloat16),
        [route_ids.T],
        [],
        "table",
        AHEAD,
        8,
    )
    rows = call(
        dispatch_kernel,
        jax.ShapeDtypeStruct((n, width), jnp.bfloat16),
        [tokens, norm_gain.reshape(1, width), table],
        [],
        "dispatch",
        2 * n * tok_rows * width,
        16,
    )
    sent = call(spread_kernel, flat, [swap, rows], [], "spread", 2 * n * 256 * width, 16)
    received = exchange(sent)
    pick_shape = jax.ShapeDtypeStruct((tok_rows, n), jnp.bfloat16)
    picks = call(
        lambda *refs: picks_kernel(capacity, *refs),
        [pick_shape] * top_count,
        [route_ids],
        [],
        "picks",
        2 * n * tok_rows * tok_rows,
        8,
    )
    result = call(
        products_kernel,
        flat,
        [swap, received, w_gate[0], w_up[0], w_down[0]],
        [
            rows_scratch,
            pltpu.VMEM((n, hidden_width), jnp.bfloat16),
            pltpu.VMEM(flat.shape, flat.dtype),
            pltpu.SemaphoreType.DMA((4,)),
        ],
        "products",
        6 * n * width * hidden_width,
        28,
        out_spec=OUTSIDE,
    )
    returned = exchange(result)
    return call(
        mix_kernel,
        jax.ShapeDtypeStruct(tokens.shape, tokens.dtype),
        [swap, returned, route_weights, *picks],
        [
            rows_scratch,
            pltpu.VMEM(tokens.shape, tokens.dtype),
            pltpu.SemaphoreType.DMA((4,)),
        ],
        "mix",
        2 * top_count * n * tok_rows * width,
        20,
        out_spec=OUTSIDE,
    )


def solution(mesh):
    return jax.shard_map(
        on_device,
        mesh=mesh,
        in_specs=(
            P(("grp", "ep", "tp"), None),
            P(),
            P(("grp", "ep", "tp"), None),
            P(("grp", "ep", "tp"), None),
            P(("ep", "tp"), None, None),
            P(("ep", "tp"), None, None),
            P(("ep", "tp"), None, None),
        ),
        out_specs=P(("grp", "ep", "tp"), None),
        check_vma=False,
    )
```

```python
import jax
import jax.numpy as jnp
from jax import lax
from jax.experimental import pallas as pl
from jax.experimental.pallas import tpu as pltpu
from jax.sharding import PartitionSpec as P

LANES = 128
AXES = ("ep", "tp")
MIB = 1 << 20
AHEAD = 1 << 32
WHOLE = pl.BlockSpec(memory_space=pltpu.VMEM)
OUTSIDE = pl.BlockSpec(memory_space=pltpu.HBM)


def swap_kernel(tiles, out_ref):
    n = tiles * tiles
    row = lax.broadcasted_iota(jnp.int32, (n, n), 0)
    column = lax.broadcasted_iota(jnp.int32, (n, n), 1)
    source = lax.rem(row, tiles) * tiles + lax.div(row, tiles)
    out_ref[...] = (column == source).astype(jnp.bfloat16)


def spread_rows(table, rows_ref, out_ref):
    n, width = rows_ref.shape
    tiles = width // LANES
    span = tiles * tiles
    for g in range(0, n, 2 * tiles):
        halves = []
        for h in (g, g + tiles):
            pieces = [rows_ref[h : h + tiles, c * LANES : (c + 1) * LANES] for c in range(tiles)]
            halves.append(jnp.concatenate(pieces, 0))
        both = jnp.dot(table, jnp.concatenate(halves, 1), preferred_element_type=jnp.float32)
        both = both.astype(jnp.bfloat16)
        out_ref[g * tiles : g * tiles + span, :] = both[:, :LANES]
        out_ref[g * tiles + span : g * tiles + 2 * span, :] = both[:, LANES:]


def gather_rows(table, in_ref, rows_ref):
    n, width = rows_ref.shape
    tiles = width // LANES
    span = tiles * tiles
    for g in range(0, n, 2 * tiles):
        first = in_ref[g * tiles : g * tiles + span, :]
        second = in_ref[g * tiles + span : g * tiles + 2 * span, :]
        both = jnp.dot(
            table, jnp.concatenate([first, second], 1), preferred_element_type=jnp.float32
        ).astype(jnp.bfloat16)
        for c in range(tiles):
            part = both[c * tiles : (c + 1) * tiles]
            rows_ref[g : g + tiles, c * LANES : (c + 1) * LANES] = part[:, :LANES]
            rows_ref[g + tiles : g + 2 * tiles, c * LANES : (c + 1) * LANES] = part[:, LANES:]


def table_kernel(capacity, ids_ref, table_ref, *pick_refs):
    n, tok_rows = table_ref.shape
    row = lax.broadcasted_iota(jnp.int32, (n, tok_rows), 0)
    expert = lax.div(row, capacity)
    picks = [ids_ref[k : k + 1, :] == expert for k in range(ids_ref.shape[0])]
    named = picks[0]
    for pick in picks[1:]:
        named = named | pick
    before = lax.broadcasted_iota(jnp.int32, (tok_rows, tok_rows), 0)
    after = lax.broadcasted_iota(jnp.int32, (tok_rows, tok_rows), 1)
    earlier = (before < after).astype(jnp.bfloat16)
    rank = jnp.dot(named.astype(jnp.bfloat16), earlier, preferred_element_type=jnp.float32)
    in_slot = rank == lax.rem(row, capacity).astype(jnp.float32)
    table_ref[...] = (named & in_slot).astype(jnp.bfloat16)
    for pick, pick_ref in zip(picks, pick_refs):
        pick_ref[...] = (pick & in_slot).astype(jnp.bfloat16)


def dispatch_kernel(tokens_ref, gain_ref, table_ref, swap_ref, out_ref, rows_ref):
    values = tokens_ref[...].astype(jnp.float32)
    scale = lax.rsqrt(jnp.mean(values * values, axis=-1, keepdims=True) + 1e-06)
    normed = (values * scale * gain_ref[...]).astype(jnp.bfloat16)
    rows = jnp.dot(table_ref[...], normed, preferred_element_type=jnp.float32)
    rows_ref[...] = rows.astype(jnp.bfloat16)
    spread_rows(swap_ref[...], rows_ref, out_ref)


def products_kernel(
    swap_ref, in_ref, gate_ref, up_ref, down_ref, out_ref, rows_ref, hidden_ref
):
    width, hidden_width = gate_ref.shape
    table = swap_ref[...]
    gather_rows(table, in_ref, rows_ref)
    rows = rows_ref[...]
    step = 256
    for f in range(0, hidden_width, step):
        gate_act = jnp.dot(rows, gate_ref[:, f : f + step], preferred_element_type=jnp.float32)
        up_act = jnp.dot(rows, up_ref[:, f : f + step], preferred_element_type=jnp.float32)
        hidden_ref[:, f : f + step] = (jax.nn.silu(gate_act) * up_act).astype(jnp.bfloat16)
    hidden = hidden_ref[...]
    for d in range(0, width, step):
        part = jnp.dot(hidden, down_ref[:, d : d + step], preferred_element_type=jnp.float32)
        rows_ref[:, d : d + step] = part.astype(jnp.bfloat16)
    spread_rows(table, rows_ref, out_ref)


def mix_kernel(swap_ref, in_ref, weights_ref, *refs):
    *pick_refs, out_hbm, rows_ref, mixed_ref, sems = refs
    width = mixed_ref.shape[1]
    gather_rows(swap_ref[...], in_ref, rows_ref)
    top_count, tok_rows = weights_ref.shape
    padding = jnp.zeros((8 - top_count, tok_rows), jnp.float32)
    weights = jnp.concatenate([weights_ref[...], padding], 0).T
    step = width // sems.shape[0]
    copies = []
    for i in range(sems.shape[0]):
        columns = slice(i * step, (i + 1) * step)
        total = None
        for k, pick_ref in enumerate(pick_refs):
            picked = lax.dot_general(
                pick_ref[...],
                rows_ref[:, columns],
                (((0,), (0,)), ((), ())),
                preferred_element_type=jnp.float32,
            )
            term = picked * weights[:, k : k + 1]
            total = term if total is None else total + term
        mixed_ref[:, columns] = total.astype(mixed_ref.dtype)
        copy = pltpu.make_async_copy(mixed_ref.at[:, columns], out_hbm.at[:, columns], sems.at[i])
        copy.start()
        copies.append(copy)
    for copy in copies:
        copy.wait()


def on_device(tokens, norm_gain, route_ids, route_weights, w_gate, w_up, w_down):
    tok_rows, width = tokens.shape
    top_count = route_ids.shape[1]
    hidden_width = w_gate.shape[2]
    experts = lax.axis_size("ep") * lax.axis_size("tp")
    capacity = 3 * tok_rows * top_count // (2 * experts)
    n = experts * capacity
    tiles = width // LANES
    flat = jax.ShapeDtypeStruct((n * tiles, LANES), jnp.bfloat16)
    rows_scratch = pltpu.VMEM((n, width), jnp.bfloat16)

    def call(kernel, out_shape, inputs, scratch, name, flops, mib, outside=(), out_spec=WHOLE):
        many = isinstance(out_shape, (list, tuple))
        return pl.pallas_call(
            kernel,
            out_shape=out_shape,
            in_specs=[OUTSIDE if i in outside else WHOLE for i in range(len(inputs))],
            out_specs=[out_spec] * len(out_shape) if many else out_spec,
            scratch_shapes=scratch,
            name=name,
            cost_estimate=pl.CostEstimate(flops=flops, bytes_accessed=4 * MIB, transcendentals=0),
            compiler_params=pltpu.CompilerParams(vmem_limit_bytes=mib * MIB),
        )(*inputs)

    def exchange(rows):
        blocks = rows.reshape(experts, capacity * tiles, LANES)
        moved = lax.all_to_all(blocks, AXES, split_axis=0, concat_axis=0, tiled=True)
        return moved.reshape(n * tiles, LANES)

    swap = call(
        lambda ref: swap_kernel(tiles, ref),
        jax.ShapeDtypeStruct((tiles * tiles, tiles * tiles), jnp.bfloat16),
        [],
        [],
        "swap",
        AHEAD,
        4,
    )
    table, *picks = call(
        lambda *refs: table_kernel(capacity, *refs),
        [jax.ShapeDtypeStruct((n, tok_rows), jnp.bfloat16)] * (1 + top_count),
        [route_ids.T],
        [],
        "table",
        2 * n * tok_rows * tok_rows,
        8,
    )
    sent = call(
        dispatch_kernel,
        flat,
        [tokens, norm_gain.reshape(1, width), table, swap],
        [rows_scratch],
        "dispatch",
        AHEAD,
        16,
    )
    received = exchange(sent)
    result = call(
        products_kernel,
        flat,
        [swap, received, w_gate[0], w_up[0], w_down[0]],
        [
            rows_scratch,
            pltpu.VMEM((n, hidden_width), jnp.bfloat16),
        ],
        "products",
        6 * n * width * hidden_width,
        28,
    )
    returned = exchange(result)
    return call(
        mix_kernel,
        jax.ShapeDtypeStruct(tokens.shape, tokens.dtype),
        [swap, returned, route_weights.T, *picks],
        [
            rows_scratch,
            pltpu.VMEM(tokens.shape, tokens.dtype),
            pltpu.SemaphoreType.DMA((4,)),
        ],
        "mix",
        2 * top_count * n * tok_rows * width,
        20,
        out_spec=OUTSIDE,
    )


def solution(mesh):
    return jax.shard_map(
        on_device,
        mesh=mesh,
        in_specs=(
            P(("grp", "ep", "tp"), None),
            P(),
            P(("grp", "ep", "tp"), None),
            P(("grp", "ep", "tp"), None),
            P(("ep", "tp"), None, None),
            P(("ep", "tp"), None, None),
            P(("ep", "tp"), None, None),
        ),
        out_specs=P(("grp", "ep", "tp"), None),
        check_vma=False,
    )
```

```python
import jax
import jax.numpy as jnp
from jax import lax
from jax.experimental import pallas as pl
from jax.experimental.pallas import tpu as pltpu
from jax.sharding import PartitionSpec as P

LANES = 128
AXES = ("ep", "tp")
MIB = 1 << 20
AHEAD = 1 << 32
WHOLE = pl.BlockSpec(memory_space=pltpu.VMEM)
OUTSIDE = pl.BlockSpec(memory_space=pltpu.HBM)


def swap_kernel(tiles, out_ref):
    n = tiles * tiles
    row = lax.broadcasted_iota(jnp.int32, (n, n), 0)
    column = lax.broadcasted_iota(jnp.int32, (n, n), 1)
    source = lax.rem(row, tiles) * tiles + lax.div(row, tiles)
    out_ref[...] = (column == source).astype(jnp.bfloat16)


def spread_rows(table, rows_ref, out_ref):
    n, width = rows_ref.shape
    tiles = width // LANES
    span = tiles * tiles
    for g in range(0, n, 2 * tiles):
        halves = []
        for h in (g, g + tiles):
            pieces = [rows_ref[h : h + tiles, c * LANES : (c + 1) * LANES] for c in range(tiles)]
            halves.append(jnp.concatenate(pieces, 0))
        both = jnp.dot(table, jnp.concatenate(halves, 1), preferred_element_type=jnp.float32)
        both = both.astype(jnp.bfloat16)
        out_ref[g * tiles : g * tiles + span, :] = both[:, :LANES]
        out_ref[g * tiles + span : g * tiles + 2 * span, :] = both[:, LANES:]


def gather_rows(table, in_ref, rows_ref):
    n, width = rows_ref.shape
    tiles = width // LANES
    span = tiles * tiles
    for g in range(0, n, 2 * tiles):
        first = in_ref[g * tiles : g * tiles + span, :]
        second = in_ref[g * tiles + span : g * tiles + 2 * span, :]
        both = jnp.dot(
            table, jnp.concatenate([first, second], 1), preferred_element_type=jnp.float32
        ).astype(jnp.bfloat16)
        for c in range(tiles):
            part = both[c * tiles : (c + 1) * tiles]
            rows_ref[g : g + tiles, c * LANES : (c + 1) * LANES] = part[:, :LANES]
            rows_ref[g + tiles : g + 2 * tiles, c * LANES : (c + 1) * LANES] = part[:, LANES:]


def table_kernel(capacity, ids_ref, table_ref, picks_ref):
    n, tok_rows = table_ref.shape
    row = lax.broadcasted_iota(jnp.int32, (n, tok_rows), 0)
    expert = lax.div(row, capacity)
    picks = [ids_ref[k : k + 1, :] == expert for k in range(ids_ref.shape[0])]
    named = picks[0]
    for pick in picks[1:]:
        named = named | pick
    before = lax.broadcasted_iota(jnp.int32, (tok_rows, tok_rows), 0)
    after = lax.broadcasted_iota(jnp.int32, (tok_rows, tok_rows), 1)
    earlier = (before < after).astype(jnp.bfloat16)
    rank = jnp.dot(named.astype(jnp.bfloat16), earlier, preferred_element_type=jnp.float32)
    in_slot = rank == lax.rem(row, capacity).astype(jnp.float32)
    table_ref[...] = (named & in_slot).astype(jnp.bfloat16)
    for k, pick in enumerate(picks):
        picks_ref[:, k * tok_rows : (k + 1) * tok_rows] = (pick & in_slot).astype(jnp.bfloat16)


def dispatch_kernel(tokens_ref, gain_ref, table_ref, swap_ref, out_ref, rows_ref):
    values = tokens_ref[...].astype(jnp.float32)
    scale = lax.rsqrt(jnp.mean(values * values, axis=-1, keepdims=True) + 1e-06)
    normed = (values * scale * gain_ref[...]).astype(jnp.bfloat16)
    rows = jnp.dot(table_ref[...], normed, preferred_element_type=jnp.float32)
    rows_ref[...] = rows.astype(jnp.bfloat16)
    spread_rows(swap_ref[...], rows_ref, out_ref)


def products_kernel(
    swap_ref, in_ref, gate_ref, up_ref, down_ref, out_ref, rows_ref, hidden_ref
):
    width, hidden_width = gate_ref.shape
    table = swap_ref[...]
    gather_rows(table, in_ref, rows_ref)
    rows = rows_ref[...]
    step = 256
    for f in range(0, hidden_width, step):
        gate_act = jnp.dot(rows, gate_ref[:, f : f + step], preferred_element_type=jnp.float32)
        up_act = jnp.dot(rows, up_ref[:, f : f + step], preferred_element_type=jnp.float32)
        hidden_ref[:, f : f + step] = (jax.nn.silu(gate_act) * up_act).astype(jnp.bfloat16)
    hidden = hidden_ref[...]
    for d in range(0, width, step):
        part = jnp.dot(hidden, down_ref[:, d : d + step], preferred_element_type=jnp.float32)
        rows_ref[:, d : d + step] = part.astype(jnp.bfloat16)
    spread_rows(table, rows_ref, out_ref)


def mix_kernel(swap_ref, in_ref, weights_ref, picks_ref, out_hbm, rows_ref, mixed_ref, sems):
    width = mixed_ref.shape[1]
    gather_rows(swap_ref[...], in_ref, rows_ref)
    top_count, tok_rows = weights_ref.shape
    padding = jnp.zeros((8 - top_count, tok_rows), jnp.float32)
    weights = jnp.concatenate([weights_ref[...], padding], 0).T
    step = width // sems.shape[0]
    copies = []
    for i in range(sems.shape[0]):
        columns = slice(i * step, (i + 1) * step)
        picked = lax.dot_general(
            picks_ref[...],
            rows_ref[:, columns],
            (((0,), (0,)), ((), ())),
            preferred_element_type=jnp.float32,
        )
        total = None
        for k in range(top_count):
            term = picked[k * tok_rows : (k + 1) * tok_rows] * weights[:, k : k + 1]
            total = term if total is None else total + term
        mixed_ref[:, columns] = total.astype(mixed_ref.dtype)
        copy = pltpu.make_async_copy(mixed_ref.at[:, columns], out_hbm.at[:, columns], sems.at[i])
        copy.start()
        copies.append(copy)
    for copy in copies:
        copy.wait()


def on_device(tokens, norm_gain, route_ids, route_weights, w_gate, w_up, w_down):
    tok_rows, width = tokens.shape
    top_count = route_ids.shape[1]
    hidden_width = w_gate.shape[2]
    experts = lax.axis_size("ep") * lax.axis_size("tp")
    capacity = 3 * tok_rows * top_count // (2 * experts)
    n = experts * capacity
    tiles = width // LANES
    flat = jax.ShapeDtypeStruct((n * tiles, LANES), jnp.bfloat16)
    rows_scratch = pltpu.VMEM((n, width), jnp.bfloat16)

    def call(kernel, out_shape, inputs, scratch, name, flops, mib, outside=(), out_spec=WHOLE):
        many = isinstance(out_shape, (list, tuple))
        return pl.pallas_call(
            kernel,
            out_shape=out_shape,
            in_specs=[OUTSIDE if i in outside else WHOLE for i in range(len(inputs))],
            out_specs=[out_spec] * len(out_shape) if many else out_spec,
            scratch_shapes=scratch,
            name=name,
            cost_estimate=pl.CostEstimate(flops=flops, bytes_accessed=4 * MIB, transcendentals=0),
            compiler_params=pltpu.CompilerParams(vmem_limit_bytes=mib * MIB),
        )(*inputs)

    def exchange(rows):
        blocks = rows.reshape(experts, capacity * tiles, LANES)
        moved = lax.all_to_all(blocks, AXES, split_axis=0, concat_axis=0, tiled=True)
        return moved.reshape(n * tiles, LANES)

    swap = call(
        lambda ref: swap_kernel(tiles, ref),
        jax.ShapeDtypeStruct((tiles * tiles, tiles * tiles), jnp.bfloat16),
        [],
        [],
        "swap",
        AHEAD,
        4,
    )
    table, picks = call(
        lambda *refs: table_kernel(capacity, *refs),
        [
            jax.ShapeDtypeStruct((n, tok_rows), jnp.bfloat16),
            jax.ShapeDtypeStruct((n, top_count * tok_rows), jnp.bfloat16),
        ],
        [route_ids.T],
        [],
        "table",
        2 * n * tok_rows * tok_rows,
        8,
    )
    sent = call(
        dispatch_kernel,
        flat,
        [tokens, norm_gain.reshape(1, width), table, swap],
        [rows_scratch],
        "dispatch",
        AHEAD,
        16,
    )
    received = exchange(sent)
    result = call(
        products_kernel,
        flat,
        [swap, received, w_gate[0], w_up[0], w_down[0]],
        [
            rows_scratch,
            pltpu.VMEM((n, hidden_width), jnp.bfloat16),
        ],
        "products",
        6 * n * width * hidden_width,
        28,
    )
    returned = exchange(result)
    return call(
        mix_kernel,
        jax.ShapeDtypeStruct(tokens.shape, tokens.dtype),
        [swap, returned, route_weights.T, picks],
        [
            rows_scratch,
            pltpu.VMEM(tokens.shape, tokens.dtype),
            pltpu.SemaphoreType.DMA((2,)),
        ],
        "mix",
        2 * top_count * n * tok_rows * width,
        20,
        out_spec=OUTSIDE,
    )


def solution(mesh):
    return jax.shard_map(
        on_device,
        mesh=mesh,
        in_specs=(
            P(("grp", "ep", "tp"), None),
            P(),
            P(("grp", "ep", "tp"), None),
            P(("grp", "ep", "tp"), None),
            P(("ep", "tp"), None, None),
            P(("ep", "tp"), None, None),
            P(("ep", "tp"), None, None),
        ),
        out_specs=P(("grp", "ep", "tp"), None),
        check_vma=False,
    )
```

```python
import jax
import jax.numpy as jnp
from jax import lax
from jax.experimental import pallas as pl
from jax.experimental.pallas import tpu as pltpu
from jax.sharding import PartitionSpec as P

LANES = 128
AXES = ("ep", "tp")
MIB = 1 << 20
AHEAD = 1 << 32
WHOLE = pl.BlockSpec(memory_space=pltpu.VMEM)
OUTSIDE = pl.BlockSpec(memory_space=pltpu.HBM)


def swap_kernel(tiles, out_ref):
    n = tiles * tiles
    row = lax.broadcasted_iota(jnp.int32, (n, n), 0)
    column = lax.broadcasted_iota(jnp.int32, (n, n), 1)
    source = lax.rem(row, tiles) * tiles + lax.div(row, tiles)
    out_ref[...] = (column == source).astype(jnp.bfloat16)


def spread_rows(table, rows_ref, out_ref):
    n, width = rows_ref.shape
    tiles = width // LANES
    span = tiles * tiles
    for g in range(0, n, 2 * tiles):
        halves = []
        for h in (g, g + tiles):
            pieces = [rows_ref[h : h + tiles, c * LANES : (c + 1) * LANES] for c in range(tiles)]
            halves.append(jnp.concatenate(pieces, 0))
        both = jnp.dot(table, jnp.concatenate(halves, 1), preferred_element_type=jnp.float32)
        both = both.astype(jnp.bfloat16)
        out_ref[g * tiles : g * tiles + span, :] = both[:, :LANES]
        out_ref[g * tiles + span : g * tiles + 2 * span, :] = both[:, LANES:]


def gather_rows(table, in_ref, rows_ref):
    n, width = rows_ref.shape
    tiles = width // LANES
    span = tiles * tiles
    for g in range(0, n, 2 * tiles):
        first = in_ref[g * tiles : g * tiles + span, :]
        second = in_ref[g * tiles + span : g * tiles + 2 * span, :]
        both = jnp.dot(
            table, jnp.concatenate([first, second], 1), preferred_element_type=jnp.float32
        ).astype(jnp.bfloat16)
        for c in range(tiles):
            part = both[c * tiles : (c + 1) * tiles]
            rows_ref[g : g + tiles, c * LANES : (c + 1) * LANES] = part[:, :LANES]
            rows_ref[g + tiles : g + 2 * tiles, c * LANES : (c + 1) * LANES] = part[:, LANES:]


def table_kernel(capacity, ids_ref, table_ref, picks_ref):
    n, tok_rows = table_ref.shape
    row = lax.broadcasted_iota(jnp.int32, (n, tok_rows), 0)
    expert = lax.div(row, capacity)
    picks = [ids_ref[k : k + 1, :] == expert for k in range(ids_ref.shape[0])]
    named = picks[0]
    for pick in picks[1:]:
        named = named | pick
    before = lax.broadcasted_iota(jnp.int32, (tok_rows, tok_rows), 0)
    after = lax.broadcasted_iota(jnp.int32, (tok_rows, tok_rows), 1)
    earlier = (before < after).astype(jnp.bfloat16)
    rank = jnp.dot(named.astype(jnp.bfloat16), earlier, preferred_element_type=jnp.float32)
    in_slot = rank == lax.rem(row, capacity).astype(jnp.float32)
    table_ref[...] = (named & in_slot).astype(jnp.bfloat16)
    for k, pick in enumerate(picks):
        picks_ref[:, k * tok_rows : (k + 1) * tok_rows] = (pick & in_slot).astype(jnp.bfloat16)


def dispatch_kernel(tokens_ref, gain_ref, table_ref, swap_ref, out_ref, rows_ref):
    values = tokens_ref[...].astype(jnp.float32)
    scale = lax.rsqrt(jnp.mean(values * values, axis=-1, keepdims=True) + 1e-06)
    normed = (values * scale * gain_ref[...]).astype(jnp.bfloat16)
    rows = jnp.dot(table_ref[...], normed, preferred_element_type=jnp.float32)
    rows_ref[...] = rows.astype(jnp.bfloat16)
    spread_rows(swap_ref[...], rows_ref, out_ref)


def products_kernel(
    swap_ref, in_ref, gate_ref, up_ref, down_ref, out_ref, rows_ref, hidden_ref
):
    width, hidden_width = gate_ref.shape
    table = swap_ref[...]
    gather_rows(table, in_ref, rows_ref)
    rows = rows_ref[...]
    step = 256
    for f in range(0, hidden_width, step):
        gate_act = jnp.dot(rows, gate_ref[:, f : f + step], preferred_element_type=jnp.float32)
        up_act = jnp.dot(rows, up_ref[:, f : f + step], preferred_element_type=jnp.float32)
        hidden_ref[:, f : f + step] = (jax.nn.silu(gate_act) * up_act).astype(jnp.bfloat16)
    hidden = hidden_ref[...]
    for d in range(0, width, step):
        part = jnp.dot(hidden, down_ref[:, d : d + step], preferred_element_type=jnp.float32)
        rows_ref[:, d : d + step] = part.astype(jnp.bfloat16)
    spread_rows(table, rows_ref, out_ref)


def mix_kernel(swap_ref, in_ref, weights_ref, picks_ref, out_hbm, rows_ref, mixed_ref, sems):
    width = mixed_ref.shape[1]
    gather_rows(swap_ref[...], in_ref, rows_ref)
    top_count, tok_rows = weights_ref.shape
    padding = jnp.zeros((8 - top_count, tok_rows), jnp.float32)
    weights = jnp.concatenate([weights_ref[...], padding], 0).T
    step = width // sems.shape[0]
    copies = []
    for i in range(sems.shape[0]):
        columns = slice(i * step, (i + 1) * step)
        picked = lax.dot_general(
            picks_ref[...],
            rows_ref[:, columns],
            (((0,), (0,)), ((), ())),
            preferred_element_type=jnp.float32,
        )
        total = None
        for k in range(top_count):
            term = picked[k * tok_rows : (k + 1) * tok_rows] * weights[:, k : k + 1]
            total = term if total is None else total + term
        mixed_ref[:, columns] = total.astype(mixed_ref.dtype)
        copy = pltpu.make_async_copy(mixed_ref.at[:, columns], out_hbm.at[:, columns], sems.at[i])
        copy.start()
        copies.append(copy)
    for copy in copies:
        copy.wait()


def on_device(tokens, norm_gain, route_ids, route_weights, w_gate, w_up, w_down):
    tok_rows, width = tokens.shape
    top_count = route_ids.shape[1]
    hidden_width = w_gate.shape[2]
    experts = lax.axis_size("ep") * lax.axis_size("tp")
    capacity = 3 * tok_rows * top_count // (2 * experts)
    n = experts * capacity
    tiles = width // LANES
    flat = jax.ShapeDtypeStruct((n * tiles, LANES), jnp.bfloat16)
    rows_scratch = pltpu.VMEM((n, width), jnp.bfloat16)

    def call(kernel, out_shape, inputs, scratch, name, flops, mib, outside=(), out_spec=WHOLE, flags=None):
        many = isinstance(out_shape, (list, tuple))
        return pl.pallas_call(
            kernel,
            out_shape=out_shape,
            in_specs=[OUTSIDE if i in outside else WHOLE for i in range(len(inputs))],
            out_specs=[out_spec] * len(out_shape) if many else out_spec,
            scratch_shapes=scratch,
            name=name,
            cost_estimate=pl.CostEstimate(flops=flops, bytes_accessed=4 * MIB, transcendentals=0),
            compiler_params=pltpu.CompilerParams(vmem_limit_bytes=mib * MIB, flags=flags),
        )(*inputs)

    def exchange(rows):
        blocks = rows.reshape(experts, capacity * tiles, LANES)
        moved = lax.all_to_all(blocks, AXES, split_axis=0, concat_axis=0, tiled=True)
        return moved.reshape(n * tiles, LANES)

    swap = call(
        lambda ref: swap_kernel(tiles, ref),
        jax.ShapeDtypeStruct((tiles * tiles, tiles * tiles), jnp.bfloat16),
        [],
        [],
        "swap",
        AHEAD,
        4,
    )
    table, picks = call(
        lambda *refs: table_kernel(capacity, *refs),
        [
            jax.ShapeDtypeStruct((n, tok_rows), jnp.bfloat16),
            jax.ShapeDtypeStruct((n, top_count * tok_rows), jnp.bfloat16),
        ],
        [route_ids.T],
        [],
        "table",
        2 * n * tok_rows * tok_rows,
        8,
    )
    sent = call(
        dispatch_kernel,
        flat,
        [tokens, norm_gain.reshape(1, width), table, swap],
        [rows_scratch],
        "dispatch",
        AHEAD,
        16,
    )
    received = exchange(sent)
    result = call(
        products_kernel,
        flat,
        [swap, received, w_gate[0], w_up[0], w_down[0]],
        [
            rows_scratch,
            pltpu.VMEM((n, hidden_width), jnp.bfloat16),
        ],
        "products",
        6 * n * width * hidden_width,
        28,
    )
    returned = exchange(result)
    return call(
        mix_kernel,
        jax.ShapeDtypeStruct(tokens.shape, tokens.dtype),
        [swap, returned, route_weights.T, picks],
        [
            rows_scratch,
            pltpu.VMEM(tokens.shape, tokens.dtype),
            pltpu.SemaphoreType.DMA((2,)),
        ],
        "mix",
        2 * top_count * n * tok_rows * width,
        20,
        out_spec=OUTSIDE,
    )


def solution(mesh):
    return jax.shard_map(
        on_device,
        mesh=mesh,
        in_specs=(
            P(("grp", "ep", "tp"), None),
            P(),
            P(("grp", "ep", "tp"), None),
            P(("grp", "ep", "tp"), None),
            P(("ep", "tp"), None, None),
            P(("ep", "tp"), None, None),
            P(("ep", "tp"), None, None),
        ),
        out_specs=P(("grp", "ep", "tp"), None),
        check_vma=False,
    )
```
